32 devices in a mesh: sp: 4 (over z), tp: 8 (over y, x, core).
Axes of the slice: x: 2, y: 2, z: 4, core: 2. Of those that a mesh axis runs over, the one named last changes fastest.
Arguments:
- token_values: bfloat16 [1024, 2048], P('sp', 'tp'), may hold values from -6 to 6
- write_keys: bfloat16 [1024, 1024], P('sp', 'tp'), may hold values from -0.4375 to 0.4375
- read_keys: bfloat16 [1024, 1024], P('sp', 'tp'), may hold values from -0.4375 to 0.4375
- log_decay: float32 [32, 1024], P('tp', 'sp'), may hold values from -0.7 to 0, as said below
- out_gate: bfloat16 [1024, 2048], P('sp', 'tp'), may hold values from -6 to 6
- out_proj: bfloat16 [4096, 2048], P(None, 'tp'), may hold values from -0.125 to 0.125
- mixed: bfloat16 [1024, 4096], P('sp'), may hold values from -6 to 6
- cotangent: bfloat16 [1024, 4096], P('sp'), may hold values from -8 to 8
- route_ids: int32 [1024, 2], P('sp'), may hold values from 0 to 3, all different within a row; in each aligned block of 256 rows (0 to 255, 256 to 511, ...) at most 192 rows name the same one
- route_weights: float32 [1024, 2], P('sp'), may hold values from 0.25 to 1
- w_gate: bfloat16 [4, 4096, 2048], P('sp', None, 'tp'), may hold values from -0.09375 to 0.09375
- w_up: bfloat16 [4, 4096, 2048], P('sp', None, 'tp'), may hold values from -0.09375 to 0.09375
- w_down: bfloat16 [4, 2048, 4096], P('sp', 'tp'), may hold values from -0.125 to 0.125
Outputs:
- value_grad: bfloat16 [1024, 2048], P('sp', 'tp')
- write_grad: bfloat16 [1024, 1024], P('sp', 'tp')
- read_grad: bfloat16 [1024, 1024], P('sp', 'tp')
- gate_grad: bfloat16 [1024, 2048], P('sp', 'tp')
- proj_grad: float32 [4096, 2048], P('sp', 'tp')
- gate_weight_grad: bfloat16 [4, 4096, 2048], P('sp', None, 'tp')
- up_weight_grad: bfloat16 [4, 4096, 2048], P('sp', None, 'tp')
- down_weight_grad: bfloat16 [4, 2048, 4096], P('sp', 'tp')
The draws below stay inside these ranges and needn't reach their ends.
Inputs may be any that keep to these rules, and one draw needn't show every extreme that they name: `route_ids`: each row names 2 different experts. Within the rows of one device no expert is named more than 192 times, and in every draw some expert is named exactly 192 times by the rows of some device. `log_decay`: every entry is negative.
All inputs are finite; a program needn't handle non-finite values.
Results may differ from the reference program's by a relative error of at most 0.019.
Values may be sent and summed in bfloat16 or wider, within the bound.
No kernel may reach another device: no remote copies, remote signals or barrier semaphores. Data moves between devices by JAX's collectives and lax.ppermute only.
A program may use at most 128 MiB of HBM per device.

```python
import math
import jax
import jax.numpy as jnp
import numpy as np
from jax import lax

D = 4096
GROUPS = 8
HEAD_DIM = 64
STATE = 128
HEADS = 32
INNER = 2048
EXPERT_HIDDEN_SIZE = 2048
TOP = 2
BLOCK = 64
TOK_DEV = 256
TOKENS = 1024
EXPERTS = 4
CAP = 192
N_SP = 4
N_TP = 8


def draw_log_decay(key, part):
    keys = jax.random.split(jax.random.fold_in(key, 7), 7)
    fast_share = 0.5
    fast = jax.random.uniform(keys[0], (HEADS, 1), jnp.float32) < fast_share
    fast_rate = jnp.exp(jax.random.uniform(keys[1], (HEADS, 1), jnp.float32, jnp.log(2.3 / 50.0), jnp.log(2.3 / 30.0)))
    keep = jax.random.uniform(keys[2], (HEADS, 1), jnp.float32, 0.55, 0.8)
    slow_rate = -jnp.log(keep) / TOKENS
    segment_factor = jnp.exp(jax.random.uniform(keys[3], (HEADS, TOKENS // TOK_DEV), jnp.float32, -0.45, 0.45))
    segment_factor = jnp.repeat(segment_factor, TOK_DEV, axis=1)
    token_factor = jnp.exp(jax.random.uniform(keys[4], (HEADS, TOKENS), jnp.float32, -0.6, 0.6))
    decay_speed = jnp.where(fast, fast_rate, slow_rate) * segment_factor * token_factor
    positions = jax.random.randint(keys[5], (HEADS, 2), 0, TOKENS)
    gate_intensity = jax.random.uniform(keys[6], (HEADS, 2), jnp.float32, jnp.log(0.5), jnp.log(0.8))
    places = jnp.arange(TOKENS, dtype=jnp.int32)
    dropped_tokens = places[None, None, :] == positions[:, :, None]
    decay_pulse = jnp.sum(jnp.where(dropped_tokens, gate_intensity[:, :, None], 0.0), axis=1)
    return jnp.clip(decay_pulse - decay_speed, -0.7, -1e-06).astype(jnp.float32)


def strengthened(drawn, stream_key, source, target, shards_of, factor):
    def block_of(dim):
        return (jnp.arange(drawn.shape[dim]) // (drawn.shape[dim] // shards_of)).reshape((-1,) + (1,) * (drawn.ndim - 1 - dim))

    first = jax.random.permutation(stream_key, shards_of)[block_of(target)]
    second = (block_of(target) + shards_of // 2) % shards_of
    return jnp.where((block_of(source) == first) | (block_of(source) == second), factor * drawn, drawn)


def shard_levels(own_key, dims, cuts, smallest, high):
    loudness, own = 1.0, jax.random.fold_in(own_key, 6)
    for dim, parts in cuts:
        heights = jnp.exp(jax.random.uniform(jax.random.fold_in(own, dim), (parts,), jnp.float32, smallest / len(cuts), high / len(cuts)))
        loudness = loudness * jnp.repeat(heights, dims[dim] // parts).reshape([-1 if axis == dim else 1 for axis in range(len(dims))])
    return loudness


def deal_out(stream_key, own, number, rows, number_of, top, bound, skew):
    order = jax.random.permutation(stream_key, number_of)
    crowded, usual = shares(number_of, rows * top, bound, skew, True), shares(number_of, rows * top, bound, skew, False)
    places = jnp.arange(number_of)

    def named(sizes, rotation):
        used = int((sizes > 0).sum())
        fixed = max(1, used // 4)
        passed = fixed + (places - fixed + rotation * (used - fixed)) % max(1, number_of - fixed)
        return jnp.zeros((number_of,), jnp.int32).at[order[jnp.where(places < fixed, places, passed)]].set(jnp.asarray(sizes, jnp.int32))

    sizes = jnp.where(number % 4 == 0, named(crowded, number // 4), named(usual, number - number // 4 - 1))
    mixed = jax.random.permutation(jax.random.fold_in(own, 3), number_of)
    source_of, receiver = mixed[0:number_of // 2 * 2:2], mixed[1:number_of // 2 * 2:2]
    margin = jnp.minimum(sizes[source_of] - 1, bound - sizes[receiver]) // 2
    margin = jnp.where((source_of == order[0]) | (receiver == order[0]) | (sizes[receiver] == 0), 0, jnp.maximum(margin, 0))
    passed = jax.random.randint(jax.random.fold_in(own, 4), (number_of // 2,), 0, 1 << 20) % (margin + 1)
    sizes = sizes.at[source_of].add(-passed).at[receiver].add(passed)
    items = jnp.searchsorted(jnp.cumsum(sizes), jnp.arange(rows * top), side="right").astype(jnp.int32)
    table = items.reshape(top, rows).T
    table = table[jax.random.permutation(jax.random.fold_in(own, 1), rows)]
    rotation = jax.random.randint(jax.random.fold_in(own, 2), (rows, 1), 0, top)
    return jnp.take_along_axis(table, (jnp.arange(top)[None, :] + rotation) % top, axis=1)


def shares(count, total, reach, lean, full):
    portions = [(1 << 20) // math.isqrt(rank ** lean) + 1 for rank in range(1, count + 1)]
    largest = reach if full else min(reach, max(-(-total // count), total * portions[0] // sum(portions)))
    least = 1 if total - largest >= count - 1 else 0
    holding, rest = [largest] + [least] * (count - 1), total - largest - least * (count - 1)
    while rest > 0:
        candidates = [i for i in range(1, count) if holding[i] < largest] or [i for i in range(1, count) if holding[i] < reach]
        whole, budget = sum([portions[i] for i in candidates]), rest
        for i in candidates:
            more = min(reach - holding[i], max(1, budget * portions[i] // whole), rest)
            holding[i] = holding[i] + more
            rest = rest - more
    return np.array(holding)


def centred(key, extent, scale, most, cuts=(), held_as=jnp.bfloat16):
    level = shard_levels(key, extent, cuts, -0.22, 0.18) if cuts else 1.0
    array = jax.random.normal(key, extent, jnp.float32) * scale * level
    return jnp.minimum(jnp.maximum(array, -most), most).astype(held_as)


def gaussian_with(stream_key, shape, deviation, most, shards, heavy, held_as=jnp.bfloat16):
    result = deviation * jax.random.normal(stream_key, shape, jnp.float32)
    if shards:
        result = result * shard_levels(stream_key, shape, shards, -0.22, 0.18)
    return jnp.clip(strengthened(result, jax.random.fold_in(stream_key, 3), *heavy), -most, most).astype(held_as)


def setup_inputs(seed: int = 0) -> dict:
    splits = jax.random.split(jax.random.key(seed), 14)
    token_values = centred(splits[0], (TOKENS, INNER), 1.0, 6.0, ((0, 4), (1, 8)))
    write_keys = centred(splits[1], (TOKENS, GROUPS * STATE), ((TOKENS * STATE // 4) ** -0.25), 0.4375, ((0, 4), (1, 8)))
    read_keys = centred(splits[2], (TOKENS, GROUPS * STATE), ((TOKENS * STATE // 4) ** -0.25), 0.4375, ((0, 4), (1, 8)))
    log_decay = draw_log_decay(jax.random.fold_in(splits[13], 71), 0)
    out_gate = centred(splits[4], (TOKENS, INNER), 1.0, 6.0, ((0, 4), (1, 8)))
    out_proj = centred(splits[5], (D, INNER), INNER ** -0.5, 0.125, ((1, 8),))
    mixed = centred(splits[6], (TOKENS, D), 1.0, 6.0, ((0, 4),))
    cotangent = gaussian_with(splits[7], (TOKENS, D), 1.0, 8.0, ((0, 4),), (0, 1, 4, 2.0))
    route_ids_keys = jax.random.split(jax.random.fold_in(splits[8], 1), TOKENS // TOK_DEV)
    route_ids_turns = jax.random.permutation(jax.random.fold_in(splits[8], 3), TOKENS // TOK_DEV)
    route_ids = jax.vmap(lambda own, number: deal_out(jax.random.fold_in(splits[8], 2), own, number, TOK_DEV, EXPERTS, TOP, CAP, 2))(route_ids_keys, route_ids_turns).reshape((TOKENS, TOP))
    route_weights = jnp.clip(0.25 + 0.75 * jax.random.uniform(splits[9], (TOKENS, TOP), jnp.float32) ** shard_levels(splits[9], (TOKENS, TOP), ((0, 4),), -0.2, 0.2), 0.25, 1.0)
    w_gate = centred(splits[10], (EXPERTS, D, EXPERT_HIDDEN_SIZE), D ** -0.5, 0.09375, ((0, 4), (2, 8)))
    w_up = centred(splits[11], (EXPERTS, D, EXPERT_HIDDEN_SIZE), D ** -0.5, 0.09375, ((0, 4), (2, 8)))
    w_down = centred(splits[12], (EXPERTS, EXPERT_HIDDEN_SIZE, D), EXPERT_HIDDEN_SIZE ** -0.5, 0.125, ((0, 4), (1, 8)))
    return {"token_values": token_values, "write_keys": write_keys, "read_keys": read_keys, "log_decay": log_decay, "out_gate": out_gate, "out_proj": out_proj, "mixed": mixed, "cotangent": cotangent, "route_ids": route_ids, "route_weights": route_weights, "w_gate": w_gate, "w_up": w_up, "w_down": w_down}


highest = lax.Precision.HIGHEST

def mix_blocks(token_values, write_keys, read_keys, log_decay, entering):
    length = token_values.shape[0]
    heads = log_decay.shape[0]
    groups = write_keys.shape[1] // STATE
    per_group = heads // groups
    blocks = length // BLOCK
    inputs = token_values.reshape(blocks, BLOCK, groups, per_group, HEAD_DIM)
    writes = write_keys.reshape(blocks, BLOCK, groups, STATE)
    reads = read_keys.reshape(blocks, BLOCK, groups, STATE)
    decay = log_decay.reshape(groups, per_group, blocks, BLOCK).transpose(2, 3, 0, 1)
    cumul = jnp.cumsum(decay, axis=1)
    spans = cumul[:, :, None] - cumul[:, None, :]
    position = jnp.arange(BLOCK, dtype=jnp.int32)
    lower = (position[:, None] >= position[None, :])[None, :, :, None, None]
    weights = jnp.exp(jnp.where(lower, spans, -jnp.inf))
    scores = jnp.einsum('clgn,csgn->clsg', reads, writes, precision=highest)
    inner = jnp.einsum('clsgr,csgrp->clgrp', scores[..., None] * weights, inputs, precision=highest)
    tails = jnp.exp(cumul[:, -1:] - cumul)
    block_states = jnp.einsum('clgn,clgrp->cgrpn', writes, inputs * tails[..., None], precision=highest)
    block_decay = jnp.exp(cumul[:, -1])

    def advance(state, pieces):
        factor, added = pieces
        return (factor[..., None, None] * state + added, state)
    final, before = lax.scan(advance, entering.reshape(groups, per_group, HEAD_DIM, STATE), (block_decay, block_states))
    carried = jnp.einsum('clgn,cgrpn->clgrp', reads, before, precision=highest) * jnp.exp(cumul)[..., None]
    return ((inner + carried).reshape(length, heads * HEAD_DIM), final.reshape(heads, HEAD_DIM, STATE))

def expert_pass(pieces):
    rows, scaled, gate_weight, up_weight, down_weight = pieces
    gate_pre = jnp.dot(rows, gate_weight, preferred_element_type=jnp.float32)
    up_pre = jnp.dot(rows, up_weight, preferred_element_type=jnp.float32)
    sigma = jax.nn.sigmoid(gate_pre)
    hidden = (jax.nn.silu(gate_pre) * up_pre).astype(jnp.bfloat16)
    grad_down = jnp.dot(hidden.T, scaled, preferred_element_type=jnp.float32).astype(jnp.bfloat16)
    d_hidden = jnp.dot(scaled, down_weight.T, preferred_element_type=jnp.float32)
    d_gate = (d_hidden * up_pre * sigma * (1.0 + gate_pre * (1.0 - sigma))).astype(jnp.bfloat16)
    d_up = (d_hidden * jax.nn.silu(gate_pre)).astype(jnp.bfloat16)
    grad_gate = jnp.dot(rows.T, d_gate, preferred_element_type=jnp.float32).astype(jnp.bfloat16)
    grad_up = jnp.dot(rows.T, d_up, preferred_element_type=jnp.float32).astype(jnp.bfloat16)
    number = rows.shape[0]
    width = gate_weight.shape[0]
    value_portion = jnp.einsum('rqf,dqf->qrd', d_gate.astype(jnp.float32).reshape(number, N_TP, -1), gate_weight.astype(jnp.float32).reshape(width, N_TP, -1))
    value_portion = value_portion + jnp.einsum('rqf,dqf->qrd', d_up.astype(jnp.float32).reshape(number, N_TP, -1), up_weight.astype(jnp.float32).reshape(width, N_TP, -1))
    rounded = lax.optimization_barrier(value_portion.astype(jnp.bfloat16)).astype(jnp.float32)
    return (grad_gate, grad_up, grad_down, lax.optimization_barrier(jnp.sum(rounded, axis=0)).astype(jnp.bfloat16))

def reference(token_values, write_keys, read_keys, log_decay, out_gate, out_proj, mixed, cotangent, route_ids, route_weights, w_gate, w_up, w_down):
    width = mixed.shape[1]
    flat_ids = route_ids.reshape(-1).astype(jnp.int32)
    pairs = flat_ids.shape[0]
    source = jnp.arange(pairs, dtype=jnp.int32) // (TOP * TOK_DEV)
    member = (flat_ids[:, None] == jnp.arange(EXPERTS, dtype=jnp.int32)[None, :]).astype(jnp.int32)
    blocked = member.reshape(N_SP, TOP * TOK_DEV, EXPERTS)
    earlier = (jnp.cumsum(blocked, axis=1).astype(jnp.int32) - blocked).reshape(pairs, EXPERTS)
    slot_index = lax.optimization_barrier(jnp.sum(earlier * member, axis=1)).astype(jnp.int32)
    target = ((flat_ids * N_SP + source) * CAP + slot_index).astype(jnp.int32)
    copies = jnp.repeat(mixed, TOP, axis=0)
    scaled = (cotangent.astype(jnp.float32)[:, None, :] * route_weights[:, :, None]).reshape(pairs, width)
    scaled = scaled.astype(jnp.bfloat16)
    places = EXPERTS * N_SP * CAP
    incoming_rows = jnp.zeros((places, width), jnp.bfloat16).at[target].set(copies).reshape(EXPERTS, N_SP * CAP, width)
    scaled_in = jnp.zeros((places, width), jnp.bfloat16).at[target].set(scaled).reshape(EXPERTS, N_SP * CAP, width)
    grad_gate, grad_up, grad_down, row_grads = lax.map(expert_pass, (incoming_rows, scaled_in, w_gate, w_up, w_down))
    picked = jnp.take(row_grads.reshape(places, width), target, axis=0).astype(jnp.float32)
    picked = picked.reshape(-1, TOP, width)
    grad_mixed = (cotangent.astype(jnp.float32) + lax.optimization_barrier(jnp.sum(picked, axis=1))).astype(jnp.bfloat16)
    out_grad = jnp.dot(grad_mixed, out_proj, preferred_element_type=jnp.float32)
    entering = jnp.zeros((log_decay.shape[0], HEAD_DIM, STATE), jnp.float32)

    def whole_mix(values_in, writes_in, reads_in, gate_in):
        mixed_heads, final = mix_blocks(values_in, writes_in, reads_in, log_decay, entering)
        return mixed_heads * jax.nn.silu(gate_in)
    gated, pullback = jax.vjp(whole_mix, token_values.astype(jnp.float32), write_keys.astype(jnp.float32), read_keys.astype(jnp.float32), out_gate.astype(jnp.float32))
    d_values, d_writes, d_reads, d_gate = pullback(out_grad)
    gated_b = gated.astype(jnp.bfloat16)
    proj_grad = jnp.dot(grad_mixed.T, gated_b, preferred_element_type=jnp.float32)
    return (d_values.astype(jnp.bfloat16), d_writes.astype(jnp.bfloat16), d_reads.astype(jnp.bfloat16), d_gate.astype(jnp.bfloat16), proj_grad, grad_gate, grad_up, grad_down)
```

```python
import jax
import jax.numpy as jnp
from jax import lax
from jax.experimental import pallas as pl
from jax.experimental.pallas import tpu as pltpu
from jax.sharding import PartitionSpec as P

HEAD_DIM = 64
STATE = 128


f32 = jnp.float32
bf16 = jnp.bfloat16
HIGH = lax.Precision.HIGHEST
VMEM = pl.BlockSpec(memory_space=pltpu.VMEM)
SMEM = pl.BlockSpec(memory_space=pltpu.SMEM)


def nn(a, b):
    return lax.dot_general(a, b, (((1,), (0,)), ((), ())), preferred_element_type=f32)


def nt(a, b):
    return lax.dot_general(a, b, (((1,), (1,)), ((), ())), preferred_element_type=f32)


def tn(a, b):
    return lax.dot_general(a, b, (((0,), (0,)), ((), ())), preferred_element_type=f32)


def sds(shape, dtype):
    return jax.ShapeDtypeStruct(shape, dtype)


def call(kernel, ins, out_shapes, flops=0, scratch=(), name=None):
    return pl.pallas_call(
        kernel,
        out_shape=out_shapes,
        in_specs=[SMEM] + [VMEM] * (len(ins) - 1),
        out_specs=[VMEM] * len(out_shapes),
        scratch_shapes=list(scratch),
        compiler_params=pltpu.CompilerParams(vmem_limit_bytes=48 * 1024 * 1024),
        cost_estimate=pl.CostEstimate(flops=flops, bytes_accessed=0, transcendentals=0),
        name=name,
    )(*ins)


class Cut:
    def __init__(self, width, n_sp, n_tp):
        share = width // n_tp
        self.strided = (share // n_sp) % 128 == 0
        self.count = n_sp if self.strided else 1
        self.chunk = share // self.count
        self.stride = width // self.count
        self.share = share

    def starts(self, j):
        return [pl.multiple_of(q * self.stride + j * self.chunk, self.chunk) for q in range(self.count)]

    def lanes(self, ref, j):
        return jnp.concatenate([ref[:, pl.ds(a, self.chunk)] for a in self.starts(j)], axis=1)

    def rows(self, ref, j):
        return jnp.concatenate([ref[pl.ds(a, self.chunk), :] for a in self.starts(j)], axis=0)

    def put_rows(self, ref, j, value):
        for q, a in enumerate(self.starts(j)):
            ref[pl.ds(a, self.chunk), :] = value[q * self.chunk : (q + 1) * self.chunk]

    def put_lanes(self, ref, j, value):
        for q, a in enumerate(self.starts(j)):
            ref[:, pl.ds(a, self.chunk)] = value[:, q * self.chunk : (q + 1) * self.chunk]


def route_rows(pos, ids_t, mixed, cut, n_sp, cap):
    tokens = mixed.shape[0]

    def kernel(pos, ids, mixed, perm, *sends):
        z, i = pos[0], pos[1]
        x = cut.lanes(mixed, i)
        before = lax.broadcasted_iota(jnp.int32, (tokens, tokens), 0)
        after = lax.broadcasted_iota(jnp.int32, (tokens, tokens), 1)
        tri = (before < after).astype(f32).astype(bf16)
        slots = lax.broadcasted_iota(jnp.int32, (cap, tokens), 0)
        first, second = ids[0:1, :], ids[1:2, :]
        for s in range(n_sp):
            e = lax.rem(z + s, n_sp)
            named = ((first == e) | (second == e)).astype(f32)
            rank = nn(jnp.broadcast_to(named, (8, tokens)).astype(bf16), tri)[0:1]
            rank = jnp.where(named > 0, rank, -1.0).astype(jnp.int32)
            hit = (slots == rank).astype(f32).astype(bf16)
            perm[s] = hit
            if s:
                sends[s - 1][...] = nn(hit, x).astype(bf16)

    outs = [sds((n_sp, cap, tokens), bf16)] + [sds((cap, cut.share), bf16)] * (n_sp - 1)
    res = call(kernel, [pos, ids_t, mixed], outs, 10**8, name="route_rows")
    return res[0], list(res[1:])


def route_scaled(pos, ids, weights, cotangent, perm, cut, n_sp, cap):
    tokens = cotangent.shape[0]

    def kernel(pos, ids, weights, cot, perm, cot_slice, *sends):
        z, i = pos[0], pos[1]
        x = cut.lanes(cot, i)
        cot_slice[...] = x
        xf = x.astype(f32)
        for s in range(1, n_sp):
            e = lax.rem(z + s, n_sp)
            scale = jnp.where(ids[:, 0:1] == e, weights[:, 0:1], 0.0) + jnp.where(
                ids[:, 1:2] == e, weights[:, 1:2], 0.0
            )
            sends[s - 1][...] = nn(perm[s], (xf * scale).astype(bf16)).astype(bf16)

    outs = [sds((tokens, cut.share), bf16)] + [sds((cap, cut.share), bf16)] * (n_sp - 1)
    res = call(kernel, [pos, ids, weights, cotangent, perm], outs, 10**8, name="route_scaled")
    return res[0], list(res[1:])


def route_own(pos, ids, weights, mixed, cotangent, perm, n_sp, cap):
    tokens, width = mixed.shape

    def kernel(pos, ids, weights, mixed, cot, perm, rows, scaled):
        z = pos[0]
        scale = jnp.where(ids[:, 0:1] == z, weights[:, 0:1], 0.0) + jnp.where(
            ids[:, 1:2] == z, weights[:, 1:2], 0.0
        )
        hit = perm[0]
        for a in range(0, width, 512):
            rows[:, a : a + 512] = nn(hit, mixed[:, a : a + 512]).astype(bf16)
            part = (cot[:, a : a + 512].astype(f32) * scale).astype(bf16)
            scaled[:, a : a + 512] = nn(hit, part).astype(bf16)

    outs = [sds((cap, width), bf16)] * 2
    return call(
        kernel, [pos, ids, weights, mixed, cotangent, perm], outs, 8 * 10**8, name="route_own"
    )


def combine(pos, perm, cot_slice, returned, cut, n_sp):
    tokens = cot_slice.shape[0]
    half = tokens // 2

    def kernel(pos, perm, cot, *refs):
        rets, outs = refs[:n_sp], refs[n_sp:]
        z = pos[0]
        total = cot[...].astype(f32)
        add = tn(perm[0], rets[0][...])
        for s in range(1, n_sp):
            add = add + tn(perm[s], rets[s][...])
        gm = (total + add).astype(bf16)
        outs[0][...] = gm[:half]
        outs[1][...] = gm[half:]
        if cut.strided:
            outs[-1][...] = gm
            for s in range(n_sp):
                a = pl.multiple_of(lax.rem(z + s, n_sp) * cut.chunk, cut.chunk)
                outs[2 + s][...] = outs[-1][:, pl.ds(a, cut.chunk)]

    outs = [sds((half, cut.share), bf16)] * 2
    scratch = []
    if cut.strided:
        outs += [sds((tokens, cut.chunk), bf16)] * n_sp
        scratch = [pltpu.VMEM((tokens, cut.share), bf16)]
    return call(
        kernel, [pos, perm, cot_slice, *returned], outs, 2 * 10**8, scratch, name="combine"
    )


def parts_of(own, pieces, rows_of, cut, j, k, cap):
    half = pieces[2 * k].shape[0]
    return (
        (0, cap, cut.lanes(own, j)),
        (cap, half, pieces[2 * k][...]),
        (cap + half, half, pieces[2 * k + 1][...]),
    )


def expert_up(pos, own, pieces, w_gate, w_up, cut, cap, n_tp):
    total = cap + 2 * pieces[0].shape[0]
    hidden = w_gate.shape[1]

    def kernel(pos, own, w_gate, w_up, *refs):
        pieces, (act, fac_gate, fac_up), (acc_g, acc_u) = refs[:-5], refs[-5:-2], refs[-2:]
        for k in range(n_tp):
            j = pos[1] ^ k
            wg, wu = cut.rows(w_gate, j), cut.rows(w_up, j)
            for a, m, x in parts_of(own, pieces, None, cut, j, k, cap):
                g, u = nn(x, wg), nn(x, wu)
                if k:
                    g, u = acc_g[a : a + m] + g, acc_u[a : a + m] + u
                acc_g[a : a + m], acc_u[a : a + m] = g, u
        g, u = acc_g[...], acc_u[...]
        sigma = jax.nn.sigmoid(g)
        silu = g * sigma
        act[...] = (silu * u).astype(bf16)
        fac_gate[...] = u * sigma * (1.0 + g * (1.0 - sigma))
        fac_up[...] = silu

    outs = [sds((total, hidden), bf16), sds((total, hidden), f32), sds((total, hidden), f32)]
    scratch = [pltpu.VMEM((total, hidden), f32)] * 2
    return call(
        kernel,
        [pos, own, w_gate, w_up, *pieces],
        outs,
        4 * total * own.shape[1] * hidden,
        scratch,
        name="expert_up",
    )


def expert_hidden(pos, own, pieces, w_down, fac_gate, fac_up, cut, cap, n_tp):
    total, hidden = fac_gate.shape

    def kernel(pos, own, w_down, fac_gate, fac_up, *refs):
        pieces, (d_gate, d_up), (acc,) = refs[:-3], refs[-3:-1], refs[-1:]
        for k in range(n_tp):
            j = pos[1] ^ k
            wd = cut.lanes(w_down, j)
            for a, m, x in parts_of(own, pieces, None, cut, j, k, cap):
                h = nt(x, wd)
                if k:
                    h = acc[a : a + m] + h
                acc[a : a + m] = h
        h = acc[...]
        d_gate[...] = (h * fac_gate[...]).astype(bf16)
        d_up[...] = (h * fac_up[...]).astype(bf16)

    outs = [sds((total, hidden), bf16)] * 2
    return call(
        kernel,
        [pos, own, w_down, fac_gate, fac_up, *pieces],
        outs,
        2 * total * own.shape[1] * hidden,
        [pltpu.VMEM((total, hidden), f32)],
        name="expert_hidden",
    )


def expert_value(pos, d_gate, d_up, w_gate, w_up, cut, ks):
    total = d_gate.shape[0]

    def kernel(pos, d_gate, d_up, w_gate, w_up, out):
        for n, k in enumerate(ks):
            j = pos[1] ^ k
            v = nt(d_gate[...], cut.rows(w_gate, j)) + nt(d_up[...], cut.rows(w_up, j))
            out[n] = v.astype(bf16)

    return call(
        kernel,
        [pos, d_gate, d_up, w_gate, w_up],
        [sds((len(ks), total, cut.share), bf16)],
        4 * total * d_gate.shape[1] * cut.share * len(ks),
        name="expert_value",
    )[0]


def expert_grads(pos, own, pieces, d_gate, d_up, cut, cap, n_tp):
    width, hidden = own.shape[1], d_gate.shape[1]

    def kernel(pos, own, d_gate, d_up, *refs):
        pieces, (grad_gate, grad_up) = refs[:-2], refs[-2:]
        for k in range(n_tp):
            j = pos[1] ^ k
            g = u = 0.0
            for a, m, x in parts_of(own, pieces, None, cut, j, k, cap):
                g = g + tn(x, d_gate[a : a + m])
                u = u + tn(x, d_up[a : a + m])
            cut.put_rows(grad_gate, j, g.astype(bf16))
            cut.put_rows(grad_up, j, u.astype(bf16))

    outs = [sds((width, hidden), bf16)] * 2
    return call(
        kernel,
        [pos, own, d_gate, d_up, *pieces],
        outs,
        4 * d_gate.shape[0] * width * hidden,
        name="expert_grads",
    )


def expert_down_grad(pos, own, pieces, act, cut, cap, n_tp):
    width, hidden = own.shape[1], act.shape[1]

    def kernel(pos, own, act, *refs):
        pieces, (grad_down,) = refs[:-1], refs[-1:]
        for k in range(n_tp):
            j = pos[1] ^ k
            g = 0.0
            for a, m, x in parts_of(own, pieces, None, cut, j, k, cap):
                g = g + tn(act[a : a + m], x)
            cut.put_lanes(grad_down, j, g.astype(bf16))

    return call(
        kernel,
        [pos, own, act, *pieces],
        [sds((hidden, width), bf16)],
        2 * act.shape[0] * width * hidden,
        name="expert_down_grad",
    )[0]


def group_call(kernel, pos, ins, kinds, outs, out_kinds, groups, name, flops=10**8):
    def spec(kind, shape):
        if kind == "whole":
            return pl.BlockSpec(shape, lambda g: (0,) * len(shape))
        if kind == "lanes":
            return pl.BlockSpec((shape[0], shape[1] // groups), lambda g: (0, g))
        if kind == "rows":
            return pl.BlockSpec((shape[0] // groups, shape[1]), lambda g: (g, 0))
        return pl.BlockSpec((1,) + shape[1:], lambda g: (g, 0, 0))

    return pl.pallas_call(
        kernel,
        grid=(groups,),
        out_shape=outs,
        in_specs=[SMEM] + [spec(k, a.shape) for k, a in zip(kinds, ins)],
        out_specs=[spec(k, a.shape) for k, a in zip(out_kinds, outs)],
        compiler_params=pltpu.CompilerParams(vmem_limit_bytes=48 * 1024 * 1024),
        cost_estimate=pl.CostEstimate(flops=flops, bytes_accessed=0, transcendentals=0),
        name=name,
    )(pos, *ins)


def lower(tokens):
    a = lax.broadcasted_iota(jnp.int32, (tokens, tokens), 0)
    b = lax.broadcasted_iota(jnp.int32, (tokens, tokens), 1)
    return a >= b


def sums(decay):
    mask = lower(decay.shape[1]).astype(f32)
    dims = (((1,), (1,)), ((), ()))
    cols = lax.dot_general(mask, decay, dims, precision=HIGH, preferred_element_type=f32)
    rows = lax.dot_general(decay, mask, dims, precision=HIGH, preferred_element_type=f32)
    return cols, rows


def spread(cols, width):
    lane = lax.broadcasted_iota(jnp.int32, (cols.shape[0], width), 1) // HEAD_DIM
    out = jnp.zeros((cols.shape[0], width), f32)
    for h in range(cols.shape[1]):
        out = jnp.where(lane == h, cols[:, h : h + 1], out)
    return out


def heads_down(rows):
    return jnp.concatenate(
        [jnp.broadcast_to(rows[h : h + 1], (HEAD_DIM, rows.shape[1])) for h in range(rows.shape[0])],
        axis=0,
    )


def only(x, h):
    lane = lax.broadcasted_iota(jnp.int32, x.shape, 1) // HEAD_DIM
    return jnp.where(lane == h, x, jnp.zeros_like(x))


def decay_of(cols, rows, h, mask):
    return jnp.exp(jnp.where(mask, cols[:, h : h + 1] - rows[h : h + 1, :], -1e30))


def gathered_state(states, totals, valid):
    out, passed = None, jnp.zeros(totals[0].shape[1:], f32)
    for s, (state, total) in enumerate(zip(states, totals), 1):
        weight = jnp.where(valid(s), jnp.exp(passed), 0.0)
        term = heads_down(weight) * state[...].astype(f32)
        out = term if out is None else out + term
        passed = passed + total[0]
    return out


def mix_ends(pos, values, writes, decay, groups):
    tokens, width = values.shape
    heads = decay.shape[1]

    def kernel(pos, values, writes, decay, ends, totals):
        cols, _ = sums(decay[0])
        last = cols[tokens - 1 : tokens, :]
        tails = spread(jnp.exp(last - cols), values.shape[1])
        ends[...] = tn((values[...].astype(f32) * tails).astype(bf16), writes[...]).astype(bf16)
        totals[0] = jnp.broadcast_to(jnp.sum(decay[0], axis=1, keepdims=True), (heads, STATE))

    outs = [sds((width, STATE), bf16), sds((groups, heads, STATE), f32)]
    return group_call(
        kernel,
        pos,
        [values, writes, decay],
        ["lanes", "lanes", "major"],
        outs,
        ["rows", "major"],
        groups,
        "mix_ends",
    )


def mix_forward(pos, values, writes, reads, decay, gate, ends, totals, groups):
    tokens, width = values.shape
    heads = decay.shape[1]
    others = len(ends)

    def kernel(pos, values, writes, reads, decay, gate, *refs):
        ends, totals, (gated, y_out, entering) = refs[:others], refs[others:-3], refs[-3:]
        z = pos[0]
        state = gathered_state(ends, totals, lambda s: z >= s).astype(bf16)
        entering[...] = state
        cols, rows = sums(decay[0])
        mask = lower(tokens)
        scores = nt(reads[...], writes[...])
        y = nt(reads[...], state) * spread(jnp.exp(cols), values.shape[1])
        for h in range(heads):
            weights = (scores * decay_of(cols, rows, h, mask)).astype(bf16)
            y = y + nn(weights, only(values[...], h))
        g = gate[...].astype(f32)
        gated[...] = (y * g * jax.nn.sigmoid(g)).astype(bf16)
        y_out[...] = y

    outs = [sds((tokens, width), bf16), sds((tokens, width), f32), sds((width, STATE), bf16)]
    return group_call(
        kernel,
        pos,
        [values, writes, reads, decay, gate, *ends, *totals],
        ["lanes"] * 3 + ["major", "lanes"] + ["rows"] * others + ["major"] * others,
        outs,
        ["lanes", "lanes", "rows"],
        groups,
        "mix_forward",
    )


def mix_out_grad(pos, pieces, out_proj, gate, reads, decay, y, cut, groups, n_tp):
    tokens, width = gate.shape
    half = tokens // 2

    def kernel(pos, out_proj, gate, reads, decay, y, *refs):
        pieces, (d_y, backs, gate_grad) = refs[:-3], refs[-3:]
        halves = []
        top = low = 0.0
        for k in range(n_tp):
            w = cut.rows(out_proj, pos[1] ^ k)
            top = top + nn(pieces[2 * k][...], w)
            low = low + nn(pieces[2 * k + 1][...], w)
        out_grad = jnp.concatenate([top, low], axis=0)
        g = gate[...].astype(f32)
        sigma = jax.nn.sigmoid(g)
        dy = out_grad * (g * sigma)
        gate_grad[...] = (out_grad * y[...] * (sigma * (1.0 + g * (1.0 - sigma)))).astype(bf16)
        cols, _ = sums(decay[0])
        leads = spread(jnp.exp(cols), gate.shape[1])
        d_y[...] = dy
        backs[...] = tn((dy * leads).astype(bf16), reads[...]).astype(bf16)

    outs = [sds((tokens, width), f32), sds((width, STATE), bf16), sds((tokens, width), bf16)]
    return group_call(
        kernel,
        pos,
        [out_proj, gate, reads, decay, y, *pieces],
        ["lanes", "lanes", "lanes", "major", "lanes"] + ["whole"] * len(pieces),
        outs,
        ["lanes", "rows", "lanes"],
        groups,
        "mix_out_grad",
        2 * tokens * width * out_proj.shape[0],
    )


def mix_inner_grads(pos, values, writes, reads, decay, d_y, entering, groups):
    tokens, width = values.shape
    heads = decay.shape[1]

    def kernel(pos, values, writes, reads, decay, d_y, entering, d_values, d_writes, d_reads):
        cols, rows = sums(decay[0])
        mask = lower(tokens)
        scores = nt(reads[...], writes[...])
        dy = d_y[...]
        dyb = dy.astype(bf16)
        d_scores = d_vals = 0.0
        for h in range(heads):
            factor = decay_of(cols, rows, h, mask)
            own = only(dyb, h)
            d_scores = d_scores + factor * nt(own, values[...])
            d_vals = d_vals + tn((scores * factor).astype(bf16), own)
        d_scores = d_scores.astype(bf16)
        leads = spread(jnp.exp(cols), values.shape[1])
        d_values[...] = d_vals
        d_writes[...] = tn(d_scores, reads[...])
        d_reads[...] = (
            nn(d_scores, writes[...]) + nn((dy * leads).astype(bf16), entering[...])
        ).astype(bf16)

    keys = writes.shape
    outs = [sds((tokens, width), f32), sds(keys, f32), sds(keys, bf16)]
    return group_call(
        kernel,
        pos,
        [values, writes, reads, decay, d_y, entering],
        ["lanes"] * 3 + ["major", "lanes", "rows"],
        outs,
        ["lanes"] * 3,
        groups,
        "mix_inner_grads",
    )


def mix_end_grads(pos, values, writes, decay, d_values, d_writes, backs, totals, groups, n_sp):
    others = len(backs)

    def kernel(pos, values, writes, decay, d_values, d_writes, *refs):
        backs, totals, (value_grad, write_grad) = refs[:others], refs[others:-2], refs[-2:]
        z = pos[0]
        state = gathered_state(backs, totals, lambda s: z + s < n_sp).astype(bf16)
        cols, _ = sums(decay[0])
        last = cols[cols.shape[0] - 1 :, :]
        tails = spread(jnp.exp(last - cols), values.shape[1])
        value_grad[...] = (d_values[...] + tails * nt(writes[...], state)).astype(bf16)
        x = (values[...].astype(f32) * tails).astype(bf16)
        write_grad[...] = (d_writes[...] + nn(x, state)).astype(bf16)

    outs = [sds(values.shape, bf16), sds(writes.shape, bf16)]
    return group_call(
        kernel,
        pos,
        [values, writes, decay, d_values, d_writes, *backs, *totals],
        ["lanes", "lanes", "major", "lanes", "lanes"] + ["rows"] * others + ["major"] * others,
        outs,
        ["lanes"] * 2,
        groups,
        "mix_end_grads",
    )


def projection_grad(pos, pieces, gated, cut, n_tp):
    width = gated[0].shape[1]
    tokens = gated[0].shape[0]
    half = pieces[0].shape[0]

    def kernel(pos, *refs):
        gated, pieces, out = refs[: len(gated_in)], refs[len(gated_in) : -1], refs[-1]
        for k in range(n_tp):
            g = 0.0
            for q in range(2):
                for n in range(half // tokens):
                    x = pieces[2 * k + q][n * tokens : (n + 1) * tokens]
                    g = g + tn(x, gated[q * (half // tokens) + n][...])
            out[pl.ds(pl.multiple_of((pos[1] ^ k) * cut.chunk, cut.chunk), cut.chunk), :] = g

    gated_in = gated
    return call(
        kernel,
        [pos, *gated, *pieces],
        [sds((n_tp * cut.chunk, width), f32)],
        2 * n_tp * cut.chunk * width * 2 * half,
        name="projection_grad",
    )[0]


def flip(x, bit):
    n = lax.axis_size("tp")
    return lax.ppermute(x, "tp", [(i, i ^ bit) for i in range(n)])


def turn(x, s):
    n = lax.axis_size("sp")
    return lax.ppermute(x, "sp", [(i, (i + s) % n) for i in range(n)])


def after(x, *tokens):
    return lax.optimization_barrier((x, *tokens))[0]


def gather_tp(a, b):
    out = {0: [a, b]}
    xa, yb = flip(a, 2), flip(b, 4)
    xb, ya = flip(b, 2), flip(a, 4)
    da, db = flip(xa, 4), flip(yb, 2)
    out[2], out[4], out[6] = [xa, xb], [ya, yb], [da, db]
    for k in (0, 2, 4, 6):
        out[k + 1] = [flip(v, 1) for v in out[k]]
    return [v for k in range(8) for v in out[k]]


def body(
    token_values,
    write_keys,
    read_keys,
    log_decay,
    out_gate,
    out_proj,
    mixed,
    cotangent,
    route_ids,
    route_weights,
    w_gate,
    w_up,
    w_down,
):
    tokens, width = mixed.shape
    n_sp, n_tp = lax.axis_size("sp"), lax.axis_size("tp")
    cap = 3 * tokens // n_sp
    cut = Cut(width, n_sp, n_tp)
    groups = write_keys.shape[1] // STATE
    decay = log_decay.reshape(groups, log_decay.shape[0] // groups, tokens)
    pos = jnp.stack([lax.axis_index("sp"), lax.axis_index("tp")]).astype(jnp.int32)
    wg, wu, wd = w_gate[0], w_up[0], w_down[0]

    def halves(blocks):
        whole = jnp.concatenate(blocks, axis=0)
        half = whole.shape[0] // 2
        return whole[:half], whole[half:]

    perm, sends = route_rows(pos, route_ids.T, mixed, cut, n_sp, cap)
    got_rows = [turn(x, s) for s, x in enumerate(sends, 1)]
    cot_slice, sends = route_scaled(pos, route_ids, route_weights, cotangent, perm, cut, n_sp, cap)
    own_rows, own_scaled = route_own(
        pos, route_ids, route_weights, mixed, cotangent, perm, n_sp, cap
    )
    sends = lax.optimization_barrier((tuple(sends), tuple(got_rows)))[0]
    got_scaled = [turn(x, s) for s, x in enumerate(sends, 1)]

    ends, total = mix_ends(pos, token_values, write_keys, decay, groups)
    ends, total = lax.optimization_barrier((ends, total, tuple(got_rows)))[:2]
    came_ends = [turn(ends, s) for s in range(1, n_sp)]
    totals = [turn(total, s) for s in range(1, n_sp)]
    gated, y, entering = mix_forward(
        pos, token_values, write_keys, read_keys, decay, out_gate, came_ends, totals, groups
    )

    row_pieces = gather_tp(*halves(got_rows))
    act, fac_gate, fac_up = expert_up(pos, own_rows, row_pieces, wg, wu, cut, cap, n_tp)
    got_scaled = lax.optimization_barrier((tuple(got_scaled), tuple(row_pieces)))[0]
    scaled_pieces = gather_tp(*halves(got_scaled))
    if cut.strided:
        gated_all = [gated] + [turn(gated, s) for s in range(1, n_sp)]
    d_gate, d_up = expert_hidden(
        pos, own_scaled, scaled_pieces, wd, fac_gate, fac_up, cut, cap, n_tp
    )

    odd = expert_value(pos, d_gate, d_up, wg, wu, cut, (1, 3, 5, 7))
    even = expert_value(pos, d_gate, d_up, wg, wu, cut, (0, 2, 4, 6))
    partner = flip(odd, 1)
    rows = n_sp * cap
    mid = rows // 2

    def pair_sum(n, a, b):
        return even[n, a:b].astype(f32) + partner[n, a:b].astype(f32)

    to_x = jnp.stack([pair_sum(1, 0, mid), pair_sum(3, 0, mid)]).astype(bf16)
    to_y = jnp.stack([pair_sum(2, mid, rows), pair_sum(3, mid, rows)]).astype(bf16)
    from_x, from_y = flip(to_x, 2), flip(to_y, 4)
    to_y2 = (pair_sum(2, 0, mid) + from_x[1].astype(f32)).astype(bf16)
    to_x2 = (pair_sum(1, mid, rows) + from_y[1].astype(f32)).astype(bf16)
    from_y2, from_x2 = flip(to_y2, 4), flip(to_x2, 2)

    def block(s):
        a = s * cap
        if a < mid:
            first, second, b = from_x[0], from_y2, a
        else:
            first, second, b = from_y[0], from_x2, a - mid
        value = pair_sum(0, a, a + cap) + first[b : b + cap].astype(f32)
        return (value + second[b : b + cap].astype(f32)).astype(bf16)

    returned = [block(0)] + [turn(block(s), -s) for s in range(1, n_sp)]
    grad_gate, grad_up = expert_grads(pos, own_rows, row_pieces, d_gate, d_up, cut, cap, n_tp)
    grad_down = expert_down_grad(pos, own_scaled, scaled_pieces, act, cut, cap, n_tp)

    gm = combine(pos, perm, cot_slice, returned, cut, n_sp)
    gm_pieces = gather_tp(gm[0], gm[1])
    if cut.strided:
        shared = [gm[2]] + [turn(gm[2 + s], s) for s in range(1, n_sp)]
        shared = lax.optimization_barrier((tuple(shared), tuple(gm_pieces)))[0]
        shared_pieces = gather_tp(*halves(shared))
        proj_grad = projection_grad(pos, shared_pieces, gated_all, cut, n_tp)
    d_y, backs, gate_grad = mix_out_grad(
        pos, gm_pieces, out_proj, out_gate, read_keys, decay, y, cut, groups, n_tp
    )
    came_backs = [turn(backs, -s) for s in range(1, n_sp)]
    d_values, d_writes, read_grad = mix_inner_grads(
        pos, token_values, write_keys, read_keys, decay, d_y, entering, groups
    )
    value_grad, write_grad = mix_end_grads(
        pos,
        token_values,
        write_keys,
        decay,
        d_values,
        d_writes,
        came_backs,
        totals[::-1],
        groups,
        n_sp,
    )
    if not cut.strided:
        whole = jnp.concatenate(
            [jnp.concatenate(gm_pieces[2 * k : 2 * k + 2], axis=0) for k in range(n_tp)], axis=1
        ).reshape(tokens, n_tp, cut.share)
        order = lax.axis_index("tp") ^ jnp.arange(n_tp, dtype=jnp.int32)
        whole = jnp.take(whole, order, axis=1).reshape(tokens, width)
        proj_grad = lax.psum_scatter(
            tn(whole, gated).astype(bf16), "sp", scatter_dimension=0, tiled=True
        ).astype(f32)
    return (
        value_grad,
        write_grad,
        read_grad,
        gate_grad,
        proj_grad,
        grad_gate[None],
        grad_up[None],
        grad_down[None],
    )


def solution(mesh):
    return jax.shard_map(
        body,
        mesh=mesh,
        in_specs=(
            P("sp", "tp"),
            P("sp", "tp"),
            P("sp", "tp"),
            P("tp", "sp"),
            P("sp", "tp"),
            P(None, "tp"),
            P("sp", None),
            P("sp", None),
            P("sp", None),
            P("sp", None),
            P("sp", None, "tp"),
            P("sp", None, "tp"),
            P("sp", "tp", None),
        ),
        out_specs=(
            P("sp", "tp"),
            P("sp", "tp"),
            P("sp", "tp"),
            P("sp", "tp"),
            P("sp", "tp"),
            P("sp", None, "tp"),
            P("sp", None, "tp"),
            P("sp", "tp", None),
        ),
        check_vma=False,
    )
```
